32 devices in a mesh: ep: 16 (over z, y, x), tp: 2 (over core).
Axes of the slice: x: 2, y: 2, z: 4, core: 2. Of those that a mesh axis runs over, the one named last changes fastest.
Arguments:
- stream: bfloat16 [512, 2048], P('ep'), may hold values from -6 to 6
- mixer_gain: float32 [2048], replicated, may hold values from 0.1 to 1.9
- gate_proj: bfloat16 [2048, 1024], P(None, 'tp'), may hold values from -0.125 to 0.125
- input_proj: bfloat16 [2048, 1024], P(None, 'tp'), may hold values from -0.125 to 0.125
- state_maps: bfloat16 [2, 2048, 256], P(None, None, 'tp'), may hold values from -0.125 to 0.125
- step_proj: bfloat16 [2048, 16], P(None, 'tp'), may hold values from -0.125 to 0.125
- step_bias: float32 [16], P('tp'), may hold values from -3 to 0.5
- decay_rate: float32 [16], P('tp'), may hold values from 0.05 to 4
- input_taps: float32 [4, 1024], P(None, 'tp'), may hold values from -3 to 3
- map_taps: float32 [2, 4, 256], P(None, None, 'tp'), may hold values from -3 to 3
- input_past: bfloat16 [512, 3, 1024], P('ep', None, 'tp'), may hold values from -6 to 6
- map_past: bfloat16 [512, 2, 3, 256], P('ep', None, None, 'tp'), may hold values from -6 to 6
- head_state: float32 [512, 16, 4096], P('ep', 'tp'), may hold values from -1.6 to 1.6
- skip_gain: float32 [16], P('tp'), may hold values from 0 to 2
- inner_gain: float32 [1024], P('tp'), may hold values from 0.1 to 1.9
- mixer_out: bfloat16 [1024, 2048], P('tp'), may hold values from -0.1875 to 0.1875
- channel_gain: float32 [2048], replicated, may hold values from 0.1 to 1.9
- expert_ids: int32 [512, 2], P('ep'), may hold values from 0 to 7, all different within a row; in each aligned block of 32 rows (0 to 31, 32 to 63, ...) at most 12 rows name the same one
- expert_weight: float32 [512, 2], P('ep'), may hold values from 0.2 to 1
- expert_gate: bfloat16 [2048, 57344], P(None, ('ep', 'tp')), may hold values from -0.125 to 0.125
- expert_up: bfloat16 [2048, 57344], P(None, ('ep', 'tp')), may hold values from -0.125 to 0.125
- expert_down: bfloat16 [57344, 2048], P(('ep', 'tp')), may hold values from -0.0625 to 0.0625
- dense_gate: bfloat16 [2048, 5632], P('tp', 'ep'), may hold values from -0.125 to 0.125
- dense_up: bfloat16 [2048, 5632], P('tp', 'ep'), may hold values from -0.125 to 0.125
- dense_down: bfloat16 [5632, 2048], P('ep', 'tp'), may hold values from -0.078125 to 0.078125
- dense_mix: float32 [2048], P('tp'), may hold values from -2 to 2
Outputs:
- stream_out: bfloat16 [512, 2048], P('ep', 'tp')
- state_out: float32 [512, 16, 4096], P('ep', 'tp')
The draws below stay inside these ranges and needn't reach their ends.
Inputs may be any that keep to these rules, and one draw needn't show every extreme that they name: `expert_ids`: each row names 2 different experts. In each aligned block of 32 rows no expert is named by more than 12 rows, and in some block one expert is named by exactly 12 rows.
All inputs are finite; a program needn't handle non-finite values.
Results may differ from the reference program's by a relative error of at most 0.015.
Values may be sent and summed in bfloat16 or wider, within the bound.
A program may use at most 128 MiB of HBM per device.

```python
import math
import jax
import jax.numpy as jnp
import numpy as np
from jax import lax

D = 2048
INNER = 1024
HEAD = 64
HEADS = 16
GROUPS = 4
NSTATE = 64
CONV = 4
EXPERTS = 8
TOP_K = 2
EXPERT_HIDDEN = 7168
DENSE_HIDDEN = 5632
SEQ_DEV = 32
BATCH = 512
CAP = 12
N_EP = 16
N_TP = 2


def steps_of(stream_key, dims, shards, low, high):
    level = 1.0
    for dim, blocks in shards:
        heights = jax.random.uniform(jax.random.fold_in(jax.random.fold_in(stream_key, 6), dim), (blocks,), jnp.float32, low / len(shards), high / len(shards))
        level = level * jnp.repeat(jnp.exp(heights), dims[dim] // blocks).reshape((-1,) + (1,) * (len(dims) - 1 - dim))
    return level


def shared_out(stream_key, own, number, rows, amount, top, limit, skew):
    ranking = jax.random.permutation(stream_key, amount)
    packed, common = portions_of(amount, rows * top, limit, skew, True), portions_of(amount, rows * top, limit, skew, False)
    places = jnp.arange(amount)

    def named(sizes, turn):
        used = int((sizes > 0).sum())
        fixed = max(1, used // 4)
        passed = fixed + (places - fixed + turn * (used - fixed)) % max(1, amount - fixed)
        return jnp.zeros((amount,), jnp.int32).at[ranking[jnp.where(places < fixed, places, passed)]].set(jnp.asarray(sizes, jnp.int32))

    sizes = jnp.where(number % 4 == 0, named(packed, number // 4), named(common, number - number // 4 - 1))
    mixed = jax.random.permutation(jax.random.fold_in(own, 3), amount)
    source_of, taker = mixed[0:amount // 2 * 2:2], mixed[1:amount // 2 * 2:2]
    slack = jnp.minimum(sizes[source_of] - 1, limit - sizes[taker]) // 2
    slack = jnp.where((source_of == ranking[0]) | (taker == ranking[0]) | (sizes[taker] == 0), 0, jnp.maximum(slack, 0))
    passed = jax.random.randint(jax.random.fold_in(own, 4), (amount // 2,), 0, 1 << 20) % (slack + 1)
    sizes = sizes.at[source_of].add(-passed).at[taker].add(passed)
    items = jnp.searchsorted(jnp.cumsum(sizes), jnp.arange(rows * top), side="right").astype(jnp.int32)
    table = items.reshape(top, rows).T
    table = table[jax.random.permutation(jax.random.fold_in(own, 1), rows)]
    turn = jax.random.randint(jax.random.fold_in(own, 2), (rows, 1), 0, top)
    return jnp.take_along_axis(table, (jnp.arange(top)[None, :] + turn) % top, axis=1)


def portions_of(amount, total, most, skew, full):
    weights = [(1 << 20) // math.isqrt(rank ** skew) + 1 for rank in range(1, amount + 1)]
    largest = most if full else min(most, max(-(-total // amount), total * weights[0] // sum(weights)))
    least = 1 if total - largest >= amount - 1 else 0
    counts, rest = [largest] + [least] * (amount - 1), total - largest - least * (amount - 1)
    while rest > 0:
        free = [i for i in range(1, amount) if counts[i] < largest] or [i for i in range(1, amount) if counts[i] < most]
        whole, left = sum([weights[i] for i in free]), rest
        for i in free:
            extra = min(most - counts[i], max(1, left * weights[i] // whole), rest)
            counts[i] = counts[i] + extra
            rest = rest - extra
    return np.array(counts)


def noise(rng, shape, width, reach, pieces=(), kind=jnp.bfloat16):
    values = width * jax.random.normal(rng, shape, jnp.float32)
    if pieces:
        values = values * steps_of(rng, shape, pieces, -0.22, 0.18)
    return jnp.clip(values, -reach, reach).astype(kind)


def setup_inputs(seed: int = 0) -> dict:
    key_list = jax.random.split(jax.random.key(seed), 27)
    stream = noise(key_list[0], (BATCH, D), 1.0, 6.0, ((0, 16),))
    mixer_gain = jnp.clip(1.0 + 0.18 * jax.random.normal(key_list[1], (D,), jnp.float32), 0.1, 1.9)
    gate_proj = noise(key_list[2], (D, INNER), D ** -0.5, 0.125, ((1, 2),))
    input_proj = noise(key_list[3], (D, INNER), D ** -0.5, 0.125, ((1, 2),))
    state_maps = noise(key_list[4], (2, D, GROUPS * NSTATE), D ** -0.5, 0.125, ((2, 2),))
    step_proj = noise(key_list[5], (D, HEADS), D ** -0.5, 0.125, ((1, 2),))
    step_bias = jnp.clip(-3.0 + 3.5 * jax.random.uniform(key_list[6], (HEADS,), jnp.float32) ** steps_of(key_list[6], (HEADS,), ((0, 2),), -0.2, 0.2), -3.0, 0.5)
    decay_rate = jnp.clip(jnp.exp(math.log(4.0) - 4.3820266 * jax.random.uniform(key_list[7], (HEADS,), jnp.float32) ** steps_of(key_list[7], (HEADS,), ((0, 2),), -0.2, 0.2)), 0.05, 4.0)
    input_taps = noise(key_list[8], (CONV, INNER), 0.5, 3.0, ((1, 2),), jnp.float32)
    map_taps = noise(key_list[9], (2, CONV, GROUPS * NSTATE), 0.5, 3.0, ((2, 2),), jnp.float32)
    input_past = noise(key_list[10], (BATCH, CONV - 1, INNER), 1.0, 6.0, ((0, 16), (2, 2)))
    map_past = noise(key_list[11], (BATCH, 2, CONV - 1, GROUPS * NSTATE), 1.0, 6.0, ((0, 16), (3, 2)))
    head_state = noise(key_list[12], (BATCH, HEADS, HEAD * NSTATE), 0.2, 1.6, ((0, 16), (1, 2)), jnp.float32)
    skip_gain = jnp.clip(2.0 * jax.random.uniform(key_list[13], (HEADS,), jnp.float32) ** steps_of(key_list[13], (HEADS,), ((0, 2),), -0.2, 0.2), 0.0, 2.0)
    inner_gain = jnp.clip(1.0 + 0.18 * jax.random.normal(key_list[14], (INNER,), jnp.float32), 0.1, 1.9)
    mixer_out = noise(key_list[15], (INNER, D), INNER ** -0.5, 0.1875, ((0, 2),))
    channel_gain = jnp.clip(1.0 + 0.18 * jax.random.normal(key_list[16], (D,), jnp.float32), 0.1, 1.9)
    expert_ids_keys = jax.random.split(jax.random.fold_in(key_list[17], 1), BATCH // SEQ_DEV)
    expert_ids_turns = jax.random.permutation(jax.random.fold_in(key_list[17], 3), BATCH // SEQ_DEV)
    expert_ids = jax.vmap(lambda own, number: shared_out(jax.random.fold_in(key_list[17], 2), own, number, SEQ_DEV, EXPERTS, TOP_K, CAP, 2))(expert_ids_keys, expert_ids_turns).reshape((BATCH, TOP_K))
    expert_weight = jnp.clip(0.2 + 0.8 * jax.random.uniform(key_list[18], (BATCH, TOP_K), jnp.float32) ** steps_of(key_list[18], (BATCH, TOP_K), ((0, 16),), -0.2, 0.2), 0.2, 1.0)
    expert_gate = noise(key_list[19], (D, EXPERTS * EXPERT_HIDDEN), D ** -0.5, 0.125, ((1, 32),))
    expert_up = noise(key_list[20], (D, EXPERTS * EXPERT_HIDDEN), D ** -0.5, 0.125, ((1, 32),))
    expert_down = noise(key_list[21], (EXPERTS * EXPERT_HIDDEN, D), EXPERT_HIDDEN ** -0.5, 0.0625, ((0, 32),))
    dense_gate = noise(key_list[22], (D, DENSE_HIDDEN), D ** -0.5, 0.125, ((0, 2), (1, 16)))
    dense_up = noise(key_list[23], (D, DENSE_HIDDEN), D ** -0.5, 0.125, ((0, 2), (1, 16)))
    dense_down = noise(key_list[24], (DENSE_HIDDEN, D), DENSE_HIDDEN ** -0.5, 0.078125, ((0, 16), (1, 2)))
    dense_mix = jnp.clip(jax.random.uniform(key_list[25], (D,), jnp.float32, -2.0, 2.0) * steps_of(key_list[25], (D,), ((0, 2),), -0.4, 0.0), -2.0, 2.0)
    return {"stream": stream, "mixer_gain": mixer_gain, "gate_proj": gate_proj, "input_proj": input_proj, "state_maps": state_maps, "step_proj": step_proj, "step_bias": step_bias, "decay_rate": decay_rate, "input_taps": input_taps, "map_taps": map_taps, "input_past": input_past, "map_past": map_past, "head_state": head_state, "skip_gain": skip_gain, "inner_gain": inner_gain, "mixer_out": mixer_out, "channel_gain": channel_gain, "expert_ids": expert_ids, "expert_weight": expert_weight, "expert_gate": expert_gate, "expert_up": expert_up, "expert_down": expert_down, "dense_gate": dense_gate, "dense_up": dense_up, "dense_down": dense_down, "dense_mix": dense_mix}


EPS = 1e-06

def rms_scale(values):
    return values * lax.rsqrt(lax.optimization_barrier(jnp.mean(values * values, axis=-1, keepdims=True)) + EPS)

def short_conv(past_rows, newest, tap_weights, along):
    window = jnp.concatenate([past_rows, jnp.expand_dims(newest, along)], axis=along).astype(jnp.float32)
    return jax.nn.silu(lax.optimization_barrier(jnp.sum(window * tap_weights, axis=along)))

def mix_heads(stream, mixer_gain, gate_proj, input_proj, state_maps, step_proj, step_bias, decay_rate, input_taps, map_taps, input_past, map_past, head_state, skip_gain, inner_gain):
    row_count = stream.shape[0]
    normed = (rms_scale(stream.astype(jnp.float32)) * mixer_gain).astype(jnp.bfloat16)
    gate_in = jnp.dot(normed, gate_proj, preferred_element_type=jnp.float32).astype(jnp.bfloat16)
    input_new = jnp.dot(normed, input_proj, preferred_element_type=jnp.float32).astype(jnp.bfloat16)
    map_new = jnp.stack([jnp.dot(normed, state_maps[0], preferred_element_type=jnp.float32), jnp.dot(normed, state_maps[1], preferred_element_type=jnp.float32)], axis=1).astype(jnp.bfloat16)
    step_size = jax.nn.softplus(jnp.dot(normed, step_proj, preferred_element_type=jnp.float32) + step_bias)
    conv_in = short_conv(input_past, input_new, input_taps, 1)
    conv_map = short_conv(map_past, map_new, map_taps, 2)
    head_count = step_size.shape[1]
    per_group = HEADS // GROUPS
    group_count = head_count // per_group
    write_map = jnp.repeat(conv_map[:, 0].reshape(row_count, group_count, NSTATE), per_group, axis=1)
    read_map = jnp.repeat(conv_map[:, 1].reshape(row_count, group_count, NSTATE), per_group, axis=1)
    values = conv_in.reshape(row_count, head_count, HEAD)
    decay_now = jnp.exp(-decay_rate * step_size)
    state_old = head_state.reshape(row_count, head_count, HEAD, NSTATE)
    state_new = decay_now[:, :, None, None] * state_old + (step_size[:, :, None] * values)[:, :, :, None] * write_map[:, :, None, :]
    gated = lax.optimization_barrier(jnp.sum(state_new * read_map[:, :, None, :], axis=3)) + skip_gain[:, None] * values
    gated = gated.reshape(row_count, head_count * HEAD) * jax.nn.silu(gate_in.astype(jnp.float32))
    inner_out = rms_scale(gated.reshape(row_count, group_count, -1)).reshape(row_count, -1) * inner_gain
    return (inner_out.astype(jnp.bfloat16), state_new.reshape(row_count, head_count, HEAD * NSTATE))

def expert_sum(ffn_in, expert_ids, expert_weight, expert_gate, expert_up, expert_down):
    total_rows, feature_count = ffn_in.shape
    hidden = expert_gate.shape[1] // EXPERTS
    row_limit = min(total_rows, N_EP * CAP)

    def visit(running, expert_index):
        matched = expert_ids == expert_index
        chosen = jnp.any(matched, axis=1)
        weight = lax.optimization_barrier(jnp.sum(jnp.where(matched, expert_weight, jnp.zeros_like(expert_weight)), axis=1))
        picked = jnp.nonzero(chosen, size=row_limit, fill_value=0)[0].astype(jnp.int32)
        is_live = jnp.arange(row_limit, dtype=jnp.int32) < jnp.sum(chosen.astype(jnp.int32))
        taken_rows = ffn_in[picked]
        first_col = (expert_index * hidden).astype(jnp.int32)
        w_gate = lax.dynamic_slice_in_dim(expert_gate, first_col, hidden, 1)
        w_up = lax.dynamic_slice_in_dim(expert_up, first_col, hidden, 1)
        w_down = lax.dynamic_slice_in_dim(expert_down, first_col, hidden, 0)
        act = (jax.nn.silu(jnp.dot(taken_rows, w_gate, preferred_element_type=jnp.float32)) * jnp.dot(taken_rows, w_up, preferred_element_type=jnp.float32)).astype(jnp.bfloat16)
        result = jnp.dot(act, w_down, preferred_element_type=jnp.float32)
        scale = jnp.where(is_live, weight[picked], jnp.zeros_like(weight[picked]))
        return (running.at[picked].add(result * scale[:, None]), None)
    start_sum = jnp.zeros((total_rows, feature_count), jnp.float32)
    total, _ = lax.scan(visit, start_sum, jnp.arange(EXPERTS, dtype=jnp.int32))
    return total

def reference(stream, mixer_gain, gate_proj, input_proj, state_maps, step_proj, step_bias, decay_rate, input_taps, map_taps, input_past, map_past, head_state, skip_gain, inner_gain, mixer_out, channel_gain, expert_ids, expert_weight, expert_gate, expert_up, expert_down, dense_gate, dense_up, dense_down, dense_mix):
    inner_out, state_out = mix_heads(stream, mixer_gain, gate_proj, input_proj, state_maps, step_proj, step_bias, decay_rate, input_taps, map_taps, input_past, map_past, head_state, skip_gain, inner_gain)
    block_cols = inner_out.shape[1] // N_TP
    mixed = jnp.zeros((stream.shape[0], mixer_out.shape[1]), jnp.float32)
    for portion in range(N_TP):
        partial_out = jnp.dot(inner_out[:, portion * block_cols:(portion + 1) * block_cols], mixer_out[portion * block_cols:(portion + 1) * block_cols], preferred_element_type=jnp.float32)
        mixed = mixed + lax.optimization_barrier(partial_out.astype(jnp.bfloat16)).astype(jnp.float32)
    hidden_mid = stream.astype(jnp.float32) + mixed
    ffn_in = (rms_scale(hidden_mid) * channel_gain).astype(jnp.bfloat16)
    routed = expert_sum(ffn_in, expert_ids, expert_weight, expert_gate, expert_up, expert_down)
    dense_act = (jax.nn.silu(jnp.dot(ffn_in, dense_gate, preferred_element_type=jnp.float32)) * jnp.dot(ffn_in, dense_up, preferred_element_type=jnp.float32)).astype(jnp.bfloat16)
    dense_res = jnp.dot(dense_act, dense_down, preferred_element_type=jnp.float32)
    stream_out = (hidden_mid + routed + jax.nn.sigmoid(dense_mix) * dense_res).astype(jnp.bfloat16)
    return (stream_out, state_out)
```

```python
import functools

import jax
import jax.numpy as jnp
from jax import lax
from jax.experimental import pallas as pl
from jax.experimental.pallas import tpu as pltpu
from jax.sharding import PartitionSpec as P

HEAD = 64
HEADS = 16
GROUPS = 4
NSTATE = 64
EXPERTS = 8
TOP_K = 2
CAP = 12


EPS = 1e-06


def rms_scale(values):
    return values * lax.rsqrt(jnp.mean(values * values, axis=-1, keepdims=True) + EPS)


def short_conv(past_rows, newest, tap_weights, along):
    window = jnp.concatenate([past_rows, jnp.expand_dims(newest, along)], axis=along).astype(
        jnp.float32
    )
    return jax.nn.silu(jnp.sum(window * tap_weights, axis=along))


def mix_heads(
    stream,
    mixer_gain,
    gate_proj,
    input_proj,
    state_maps,
    step_proj,
    step_bias,
    decay_rate,
    input_taps,
    map_taps,
    input_past,
    map_past,
    head_state,
    skip_gain,
    inner_gain,
):
    row_count = stream.shape[0]
    normed = (rms_scale(stream.astype(jnp.float32)) * mixer_gain).astype(jnp.bfloat16)
    gate_in = jnp.dot(normed, gate_proj, preferred_element_type=jnp.float32).astype(jnp.bfloat16)
    input_new = jnp.dot(normed, input_proj, preferred_element_type=jnp.float32).astype(jnp.bfloat16)
    map_new = jnp.stack(
        [
            jnp.dot(normed, state_maps[0], preferred_element_type=jnp.float32),
            jnp.dot(normed, state_maps[1], preferred_element_type=jnp.float32),
        ],
        axis=1,
    ).astype(jnp.bfloat16)
    step_size = jax.nn.softplus(
        jnp.dot(normed, step_proj, preferred_element_type=jnp.float32) + step_bias
    )
    conv_in = short_conv(input_past, input_new, input_taps, 1)
    conv_map = short_conv(map_past, map_new, map_taps, 2)
    head_count = step_size.shape[1]
    per_group = HEADS // GROUPS
    group_count = head_count // per_group
    write_map = jnp.repeat(
        conv_map[:, 0].reshape(row_count, group_count, NSTATE), per_group, axis=1
    )
    read_map = jnp.repeat(conv_map[:, 1].reshape(row_count, group_count, NSTATE), per_group, axis=1)
    values = conv_in.reshape(row_count, head_count, HEAD)
    decay_now = jnp.exp(-decay_rate * step_size)
    state_old = head_state.reshape(row_count, head_count, HEAD, NSTATE)
    state_new = (
        decay_now[:, :, None, None] * state_old
        + (step_size[:, :, None] * values)[:, :, :, None] * write_map[:, :, None, :]
    )
    gated = jnp.sum(state_new * read_map[:, :, None, :], axis=3) + skip_gain[:, None] * values
    gated = gated.reshape(row_count, head_count * HEAD) * jax.nn.silu(gate_in.astype(jnp.float32))
    inner_out = (
        rms_scale(gated.reshape(row_count, group_count, -1)).reshape(row_count, -1) * inner_gain
    )
    return (inner_out.astype(jnp.bfloat16), state_new.reshape(row_count, head_count, HEAD * NSTATE))


MESH = pl.DeviceIdType.MESH


def grid_of(ep_count):
    side = 4 if ep_count % 64 == 0 else (2 if ep_count % 4 == 0 else 1)
    return side, ep_count // (side * side)


class Place:
    def __init__(self, ep_count):
        self.side, self.line = grid_of(ep_count)
        self.ep = lax.axis_index("ep")
        self.core = lax.axis_index("tp")
        col = self.ep % self.side
        row = (self.ep // self.side) % self.side
        self.z = self.ep // (self.side * self.side)
        self.a = row * (1 - self.core) + col * self.core
        self.b = col * (1 - self.core) + row * self.core
        self.row, self.col = row, col

    def at(self, db, da, dz, core=None):
        core = self.core if core is None else core
        a = self.row * (1 - core) + self.col * core
        b = self.col * (1 - core) + self.row * core
        a = (a + da) % self.side
        b = (b + db) % self.side
        z = (self.z + dz) % self.line
        row = a * (1 - core) + b * core
        col = b * (1 - core) + a * core
        return (z * self.side + row) * self.side + col

    def near(self, db, da, dz):
        return {"ep": self.at(db, da, dz), "tp": self.core}

    def sibling(self):
        return {"ep": self.ep, "tp": 1 - self.core}

    def z_order(self):
        line = self.line
        return sorted(range(1, line), key=lambda d: (min(d, line - d), d))

    def partners(self):
        side = range(1, self.side)
        return (
            [self.near(d, 0, 0) for d in side]
            + [self.near(0, d, 0) for d in side]
            + [self.near(0, 0, d) for d in self.z_order()]
        )


def greet(targets):
    barrier = pltpu.get_barrier_semaphore()
    for target in targets:
        pl.semaphore_signal(barrier, inc=1, device_id=target, device_id_type=MESH)
    pl.semaphore_wait(barrier, len(targets))


def spread_kernel(ep_count, partial, stream, gain, meta, every, notes, kept, other, *sems):
    part_send, part_recv, note_send, note_recv, link_send, link_recv, core_send, core_recv = sems
    place = Place(ep_count)
    side, line = place.side, place.line
    half = every.shape[3]
    me = place.ep
    everyone = [{"ep": (me + d) % ep_count, "tp": place.core} for d in range(1, ep_count)]
    greet([place.sibling()] + everyone)
    sends = []

    def send(src, dst, send_sem, recv_sem, target):
        copy = pltpu.make_async_remote_copy(
            src_ref=src, dst_ref=dst, send_sem=send_sem, recv_sem=recv_sem,
            device_id=target, device_id_type=MESH,
        )
        copy.start()
        sends.append(copy)
        return copy

    swap = send(partial, other, part_send, part_recv, place.sibling())
    for d in range(1, ep_count):
        send(meta, notes.at[me], note_send.at[d - 1], note_recv.at[d - 1], everyone[d - 1])
    notes[me] = meta[...]
    swap.wait_recv()
    hidden = stream[...].astype(jnp.float32) + (
        partial[...].astype(jnp.float32) + other[...].astype(jnp.float32)
    )
    ffn_in = (rms_scale(hidden) * gain[...]).astype(jnp.bfloat16)
    first = place.core == 0
    kept[...] = jnp.where(first, hidden[:, :half], hidden[:, half:])
    every[0, me] = jnp.where(first, ffn_in[:, :half], ffn_in[:, half:])
    every[1, me] = jnp.where(first, ffn_in[:, half:], ffn_in[:, :half])

    def slot(db, da, dz):
        return ((db % side) * side + da % side) * line + dz % line

    used = [0]

    def pass_on(off, step):
        block = every.at[0, place.at(*off)]
        there = slot(*(o - s for o, s in zip(off, step)))
        send(block, block, link_send.at[used[0]], link_recv.at[there], place.near(*step))
        used[0] += 1

    def arrived(off):
        block = every.at[0, place.at(*off)]
        at = slot(*off)
        pltpu.make_async_copy(block, block, link_recv.at[at]).wait()
        send(block, every.at[1, place.at(*off)], core_send.at[at], core_recv.at[at], place.sibling())

    for dz in place.z_order():
        pass_on((0, 0, 0), (0, 0, dz))
    zs = [0] + place.z_order()
    for dz in zs:
        if dz:
            arrived((0, 0, dz))
        for d in range(1, side):
            pass_on((0, 0, dz), (0, d, 0))
        for d in range(1, side):
            pass_on((0, 0, dz), (d, 0, 0))
    for dz in zs:
        for da in range(1, side):
            arrived((0, da, dz))
            for d in range(1, side):
                pass_on((0, da, dz), (d, 0, 0))
    for dz in zs:
        for da in range(side):
            for db in range(1, side):
                arrived((db, da, dz))
    for d in range(1, ep_count):
        source = (me + ep_count - d) % ep_count
        pltpu.make_async_copy(notes.at[source], notes.at[source], note_recv.at[d - 1]).wait()
    for at in range(1, ep_count):
        dz, rest = at % line, at // line
        source = place.at(rest // side, rest % side, dz, 1 - place.core)
        block = every.at[1, source]
        pltpu.make_async_copy(block, block, core_recv.at[at]).wait()
    for copy in sends:
        copy.wait_send()


def spread(partial, stream, gain, meta):
    ep_count = lax.axis_size("ep")
    rows, width = stream.shape
    half = width // 2
    vmem = pl.BlockSpec(memory_space=pltpu.VMEM)
    dma = pltpu.SemaphoreType.DMA
    return pl.pallas_call(
        functools.partial(spread_kernel, ep_count),
        out_shape=(
            jax.ShapeDtypeStruct((2, ep_count, rows, half), jnp.bfloat16),
            jax.ShapeDtypeStruct((ep_count,) + meta.shape, jnp.float32),
            jax.ShapeDtypeStruct((rows, half), jnp.float32),
        ),
        in_specs=[vmem] * 4,
        out_specs=(vmem,) * 3,
        scratch_shapes=[
            pltpu.VMEM((rows, width), jnp.bfloat16),
            dma, dma,
            dma((ep_count,)), dma((ep_count,)),
            dma((ep_count,)), dma((ep_count,)),
            dma((ep_count,)), dma((ep_count,)),
        ],
        compiler_params=pltpu.CompilerParams(
            collective_id=1, has_side_effects=True, vmem_limit_bytes=VMEM_SMALL
        ),
        name="spread",
    )(partial, stream, gain, meta)


def collect_kernel(ep_count, own, theirs, kept, out, held, total, from_b, from_a, from_z, *sems):
    core_send, core_recv, link_send, recv_b, recv_a, recv_z = sems
    place = Place(ep_count)
    side, line = place.side, place.line
    greet([place.sibling()] + place.partners())
    zs = place.z_order() + [0]
    spots = [(db, da, dz) for dz in zs for da in range(side) for db in range(1, side)]
    spots += [(0, da, dz) for dz in zs for da in range(1, side)]
    spots += [(0, 0, dz) for dz in zs]
    sends = []

    def send(src, dst, send_sem, recv_sem, target):
        copy = pltpu.make_async_remote_copy(
            src_ref=src, dst_ref=dst, send_sem=send_sem, recv_sem=recv_sem,
            device_id=target, device_id_type=MESH,
        )
        copy.start()
        sends.append(copy)

    for at, off in enumerate(spots):
        send(
            theirs.at[place.at(*off, 1 - place.core)], held.at[at],
            core_send.at[at], core_recv.at[at], place.sibling(),
        )

    def take(ref, sem):
        pltpu.make_async_copy(ref, ref, sem).wait()
        return ref[...].astype(jnp.float32)

    for at, (db, da, dz) in enumerate(spots):
        value = own[place.at(db, da, dz)].astype(jnp.float32)
        value = value + take(held.at[at], core_recv.at[at])
        if db:
            total[at] = value.astype(jnp.bfloat16)
            send(
                total.at[at], from_b.at[db - 1, da, dz],
                link_send.at[at], recv_b.at[db - 1, da, dz], place.near(db, 0, 0),
            )
            continue
        for d in range(1, side):
            value = value + take(from_b.at[d - 1, da, dz], recv_b.at[d - 1, da, dz])
        if da:
            total[at] = value.astype(jnp.bfloat16)
            send(
                total.at[at], from_a.at[da - 1, dz],
                link_send.at[at], recv_a.at[da - 1, dz], place.near(0, da, 0),
            )
            continue
        for d in range(1, side):
            value = value + take(from_a.at[d - 1, dz], recv_a.at[d - 1, dz])
        if dz:
            total[at] = value.astype(jnp.bfloat16)
            send(
                total.at[at], from_z.at[dz - 1],
                link_send.at[at], recv_z.at[dz - 1], place.near(0, 0, dz),
            )
            continue
        for d in range(1, line):
            value = value + take(from_z.at[d - 1], recv_z.at[d - 1])
        out[...] = (kept[...] + value).astype(out.dtype)
    for copy in sends:
        copy.wait_send()


def collect(own, theirs, kept):
    ep_count = lax.axis_size("ep")
    side, line = grid_of(ep_count)
    rows, half = kept.shape
    vmem = pl.BlockSpec(memory_space=pltpu.VMEM)
    dma = pltpu.SemaphoreType.DMA
    more = max(side - 1, 1)
    block = (rows, half)
    return pl.pallas_call(
        functools.partial(collect_kernel, ep_count),
        out_shape=jax.ShapeDtypeStruct((rows, half), jnp.bfloat16),
        in_specs=[vmem] * 3,
        out_specs=vmem,
        scratch_shapes=[
            pltpu.VMEM((ep_count,) + block, jnp.bfloat16),
            pltpu.VMEM((ep_count,) + block, jnp.bfloat16),
            pltpu.VMEM((more, side, line) + block, jnp.bfloat16),
            pltpu.VMEM((more, line) + block, jnp.bfloat16),
            pltpu.VMEM((max(line - 1, 1),) + block, jnp.bfloat16),
            dma((ep_count,)), dma((ep_count,)), dma((ep_count,)),
            dma((more, side, line)), dma((more, line)), dma((max(line - 1, 1),)),
        ],
        compiler_params=pltpu.CompilerParams(
            collective_id=2, has_side_effects=True, vmem_limit_bytes=VMEM_SMALL
        ),
        name="collect",
    )(own.reshape((ep_count,) + block), theirs.reshape((ep_count,) + block), kept)


VMEM_SMALL = 40 * 1024 * 1024


def local(
    stream,
    mixer_gain,
    gate_proj,
    input_proj,
    state_maps,
    step_proj,
    step_bias,
    decay_rate,
    input_taps,
    map_taps,
    input_past,
    map_past,
    head_state,
    skip_gain,
    inner_gain,
    mixer_out,
    channel_gain,
    expert_ids,
    expert_weight,
    expert_gate,
    expert_up,
    expert_down,
    dense_gate,
    dense_up,
    dense_down,
    dense_mix,
):
    core = lax.axis_index("tp")
    first = core == 0
    swap = [(0, 1), (1, 0)]
    units = dense_gate.shape[1] // 2

    def mine(left, right):
        return jnp.where(first, left, right)

    low = jnp.concatenate([dense_gate[:, :units], dense_up[:, :units]], axis=1)
    high = jnp.concatenate([dense_gate[:, units:], dense_up[:, units:]], axis=1)
    wide_own = mine(low, high)
    wide_other = lax.ppermute(mine(high, low), "tp", swap)
    down_own = mine(dense_down[:units], dense_down[units:])
    down_other = lax.ppermute(mine(dense_down[units:], dense_down[:units]), "tp", swap)
    mix_other = lax.ppermute(dense_mix, "tp", swap)

    inner_out, state_out = mix_heads(
        stream, mixer_gain, gate_proj, input_proj, state_maps, step_proj, step_bias, decay_rate,
        input_taps, map_taps, input_past, map_past, head_state, skip_gain, inner_gain,
    )
    partial_out = jnp.dot(inner_out, mixer_out, preferred_element_type=jnp.float32)

    row_count, width = stream.shape
    half = width // 2
    named = expert_ids[:, :, None] == jnp.arange(EXPERTS, dtype=jnp.int32)
    weight = jnp.sum(jnp.where(named, expert_weight[:, :, None], 0.0), axis=1)
    hits = jnp.any(named, axis=1)
    earlier = jnp.tril(jnp.ones((row_count, row_count), jnp.bfloat16), -1)
    rank = jnp.dot(earlier, hits.astype(jnp.bfloat16), preferred_element_type=jnp.float32)
    rank = jnp.where(hits, rank, -1.0)
    lanes = -(-2 * row_count // 128) * 128
    meta = jnp.concatenate([rank.T, weight.T], axis=1)
    meta = jnp.pad(meta, ((0, 0), (0, lanes - 2 * row_count)))

    every, notes, kept = spread(
        partial_out.astype(jnp.bfloat16), stream, channel_gain[None, :], meta
    )

    ep_count = lax.axis_size("ep")
    total_rows = ep_count * row_count
    slots = ep_count * CAP
    expert = lax.axis_index("ep") // (ep_count // EXPERTS)
    notes = lax.dynamic_index_in_dim(notes, expert, 1, keepdims=False)
    rank_all = notes[:, :row_count].reshape(1, total_rows)
    weight_all = notes[:, row_count : 2 * row_count].reshape(1, total_rows)
    slot_ids = jnp.arange(slots, dtype=jnp.int32)[:, None]
    row_ids = jnp.arange(total_rows, dtype=jnp.int32)[None, :]
    match = (slot_ids // CAP == row_ids // row_count) & (
        (slot_ids % CAP).astype(jnp.float32) == rank_all
    )
    slot_weight = jnp.sum(jnp.where(match, weight_all, 0.0), axis=1, keepdims=True)
    pick = match.astype(jnp.bfloat16)
    all_own = every[0].reshape(total_rows, half)
    all_other = every[1].reshape(total_rows, half)

    def f32_dot(left, right):
        return jnp.dot(left, right, preferred_element_type=jnp.float32)

    rows_own = f32_dot(pick, all_own).astype(jnp.bfloat16)
    rows_other = f32_dot(pick, all_other).astype(jnp.bfloat16)
    rows = jnp.concatenate([mine(rows_own, rows_other), mine(rows_other, rows_own)], axis=1)
    act = (jax.nn.silu(f32_dot(rows, expert_gate)) * f32_dot(rows, expert_up)).astype(jnp.bfloat16)
    share = (f32_dot(act, expert_down) * slot_weight).astype(jnp.bfloat16)
    share_own = mine(share[:, :half], share[:, half:])
    share_other = mine(share[:, half:], share[:, :half])

    wide = f32_dot(all_own, wide_own) + f32_dot(all_other, wide_other)
    dense_act = (jax.nn.silu(wide[:, :units]) * wide[:, units:]).astype(jnp.bfloat16)

    def result(share_half, down_half, mix_half):
        spread_back = lax.dot_general(
            pick, share_half, (((0,), (0,)), ((), ())), preferred_element_type=jnp.float32
        )
        dense = f32_dot(dense_act, down_half) * jax.nn.sigmoid(mix_half)
        return (spread_back + dense).astype(jnp.bfloat16)

    updated = collect(
        result(share_own, down_own, dense_mix),
        result(share_other, down_other, mix_other),
        kept,
    )
    return (updated, state_out)


def solution(mesh):
    placed = (
        P("ep", None),
        P(),
        P(None, "tp"),
        P(None, "tp"),
        P(None, None, "tp"),
        P(None, "tp"),
        P("tp"),
        P("tp"),
        P(None, "tp"),
        P(None, None, "tp"),
        P("ep", None, "tp"),
        P("ep", None, None, "tp"),
        P("ep", "tp", None),
        P("tp"),
        P("tp"),
        P("tp", None),
        P(),
        P("ep", None),
        P("ep", None),
        P(None, ("ep", "tp")),
        P(None, ("ep", "tp")),
        P(("ep", "tp"), None),
        P("tp", "ep"),
        P("tp", "ep"),
        P("ep", "tp"),
        P("tp"),
    )
    return jax.shard_map(
        local,
        mesh=mesh,
        in_specs=placed,
        out_specs=(P("ep", "tp"), P("ep", "tp", None)),
        check_vma=False,
    )
```

```python
import functools

import jax
import jax.numpy as jnp
from jax import lax
from jax.experimental import pallas as pl
from jax.experimental.pallas import tpu as pltpu
from jax.sharding import PartitionSpec as P

HEAD = 64
HEADS = 16
GROUPS = 4
NSTATE = 64
EXPERTS = 8
TOP_K = 2
CAP = 12


EPS = 1e-06


def rms_scale(values):
    return values * lax.rsqrt(jnp.mean(values * values, axis=-1, keepdims=True) + EPS)


def short_conv(past_rows, newest, tap_weights, along):
    window = jnp.concatenate([past_rows, jnp.expand_dims(newest, along)], axis=along).astype(
        jnp.float32
    )
    return jax.nn.silu(jnp.sum(window * tap_weights, axis=along))


def three_parts(value):
    high = value.astype(jnp.bfloat16)
    rest = value - high.astype(jnp.float32)
    middle = rest.astype(jnp.bfloat16)
    return high, middle, (rest - middle.astype(jnp.float32)).astype(jnp.bfloat16)


def state_kernel(state, fed, write, read_by, decay, state_out, read, picks):
    lanes = state.shape[1]

    @pl.when(pl.program_id(0) == 0)
    def _():
        rows_of = lax.broadcasted_iota(jnp.int32, picks.shape, 0)
        owner = lax.broadcasted_iota(jnp.int32, picks.shape, 1) // NSTATE
        picks[...] = jnp.where(rows_of == owner, 1.0, 0.0).astype(jnp.bfloat16)

    width = 4 * 128
    copies = width // NSTATE
    fed_parts = three_parts(fed[...])
    write_wide = jnp.concatenate([write[...]] * copies, axis=1)
    read_wide = jnp.concatenate([read_by[...]] * copies, axis=1)
    decay_wide = jnp.concatenate([decay[...]] * (width // 128), axis=1)
    total = jnp.zeros(read.shape, jnp.float32)
    for at in range(0, lanes, width):
        cut = slice(at, at + width)
        pick = picks[:, cut]
        fed_wide = sum(
            jnp.dot(part, pick, preferred_element_type=jnp.float32) for part in fed_parts[::-1]
        )
        value = decay_wide * state[:, cut] + fed_wide * write_wide
        state_out[:, cut] = value
        for part in three_parts(value * read_wide):
            total = total + lax.dot_general(
                part, pick, (((1,), (1,)), ((), ())), preferred_element_type=jnp.float32
            )
    read[...] = total


def step_state(state, fed, write, read_by, decay):
    flat, lanes = state.shape
    rows = 64

    def block(array):
        return pl.BlockSpec((rows, array.shape[1]), lambda i: (i, 0))

    return pl.pallas_call(
        state_kernel,
        grid=(flat // rows,),
        out_shape=(
            jax.ShapeDtypeStruct(state.shape, jnp.float32),
            jax.ShapeDtypeStruct(fed.shape, jnp.float32),
        ),
        in_specs=[block(x) for x in (state, fed, write, read_by, decay)],
        out_specs=(block(state), block(fed)),
        scratch_shapes=[pltpu.VMEM((HEAD, lanes), jnp.bfloat16)],
        compiler_params=pltpu.CompilerParams(
            dimension_semantics=("arbitrary",), vmem_limit_bytes=16 * 1024 * 1024
        ),
        name="state",
    )(state, fed, write, read_by, decay)


def mix_heads(
    stream,
    mixer_gain,
    gate_proj,
    input_proj,
    state_maps,
    step_proj,
    step_bias,
    decay_rate,
    input_taps,
    map_taps,
    input_past,
    map_past,
    head_state,
    skip_gain,
    inner_gain,
):
    row_count = stream.shape[0]
    normed = (rms_scale(stream.astype(jnp.float32)) * mixer_gain).astype(jnp.bfloat16)
    gate_in = jnp.dot(normed, gate_proj, preferred_element_type=jnp.float32).astype(jnp.bfloat16)
    input_new = jnp.dot(normed, input_proj, preferred_element_type=jnp.float32).astype(jnp.bfloat16)
    map_new = jnp.stack(
        [
            jnp.dot(normed, state_maps[0], preferred_element_type=jnp.float32),
            jnp.dot(normed, state_maps[1], preferred_element_type=jnp.float32),
        ],
        axis=1,
    ).astype(jnp.bfloat16)
    step_size = jax.nn.softplus(
        jnp.dot(normed, step_proj, preferred_element_type=jnp.float32) + step_bias
    )
    conv_in = short_conv(input_past, input_new, input_taps, 1)
    conv_map = short_conv(map_past, map_new, map_taps, 2)
    head_count = step_size.shape[1]
    per_group = HEADS // GROUPS
    group_count = head_count // per_group
    values = conv_in.reshape(row_count, head_count, HEAD)
    decay_now = jnp.exp(-decay_rate * step_size)
    flat = row_count * head_count

    def by_head(maps):
        maps = maps.reshape(row_count, group_count, 1, NSTATE)
        return jnp.broadcast_to(
            maps, (row_count, group_count, per_group, NSTATE)
        ).reshape(flat, NSTATE)

    state_new, read = step_state(
        head_state.reshape(flat, HEAD * NSTATE),
        (step_size[:, :, None] * values).reshape(flat, HEAD),
        by_head(conv_map[:, 0]),
        by_head(conv_map[:, 1]),
        jnp.broadcast_to(decay_now[:, :, None], (row_count, head_count, 128)).reshape(flat, 128),
    )
    gated = read.reshape(row_count, head_count, HEAD) + skip_gain[:, None] * values
    gated = gated.reshape(row_count, head_count * HEAD) * jax.nn.silu(gate_in.astype(jnp.float32))
    inner_out = (
        rms_scale(gated.reshape(row_count, group_count, -1)).reshape(row_count, -1) * inner_gain
    )
    return (
        inner_out.astype(jnp.bfloat16),
        state_new.reshape(row_count, head_count, HEAD * NSTATE),
    )


MESH = pl.DeviceIdType.MESH


def grid_of(ep_count):
    side = 4 if ep_count % 64 == 0 else (2 if ep_count % 4 == 0 else 1)
    return side, ep_count // (side * side)


class Place:
    def __init__(self, ep_count):
        self.side, self.line = grid_of(ep_count)
        self.ep = lax.axis_index("ep")
        self.core = lax.axis_index("tp")
        col = self.ep % self.side
        row = (self.ep // self.side) % self.side
        self.z = self.ep // (self.side * self.side)
        self.a = row * (1 - self.core) + col * self.core
        self.b = col * (1 - self.core) + row * self.core
        self.row, self.col = row, col

    def at(self, db, da, dz, core=None):
        core = self.core if core is None else core
        a = self.row * (1 - core) + self.col * core
        b = self.col * (1 - core) + self.row * core
        a = (a + da) % self.side
        b = (b + db) % self.side
        z = (self.z + dz) % self.line
        row = a * (1 - core) + b * core
        col = b * (1 - core) + a * core
        return (z * self.side + row) * self.side + col

    def near(self, db, da, dz):
        return {"ep": self.at(db, da, dz), "tp": self.core}

    def sibling(self):
        return {"ep": self.ep, "tp": 1 - self.core}

    def z_order(self):
        line = self.line
        return sorted(range(1, line), key=lambda d: (min(d, line - d), d))

    def partners(self):
        side = range(1, self.side)
        return (
            [self.near(d, 0, 0) for d in side]
            + [self.near(0, d, 0) for d in side]
            + [self.near(0, 0, d) for d in self.z_order()]
        )


def greet(targets):
    barrier = pltpu.get_barrier_semaphore()
    for target in targets:
        pl.semaphore_signal(barrier, inc=1, device_id=target, device_id_type=MESH)
    pl.semaphore_wait(barrier, len(targets))


def spread_kernel(ep_count, partial, stream, gain, meta, every, notes, kept, other, *sems):
    part_send, part_recv, note_send, note_recv, link_send, link_recv, core_send, core_recv = sems
    place = Place(ep_count)
    side, line = place.side, place.line
    half = every.shape[3]
    me = place.ep
    everyone = [{"ep": (me + d) % ep_count, "tp": place.core} for d in range(1, ep_count)]
    greet([place.sibling()] + everyone)
    sends = []

    def send(src, dst, send_sem, recv_sem, target):
        copy = pltpu.make_async_remote_copy(
            src_ref=src, dst_ref=dst, send_sem=send_sem, recv_sem=recv_sem,
            device_id=target, device_id_type=MESH,
        )
        copy.start()
        sends.append(copy)
        return copy

    swap = send(partial, other, part_send, part_recv, place.sibling())
    for d in range(1, ep_count):
        send(meta, notes.at[me], note_send.at[d - 1], note_recv.at[d - 1], everyone[d - 1])
    notes[me] = meta[...]
    swap.wait_recv()
    hidden = stream[...].astype(jnp.float32) + (
        partial[...].astype(jnp.float32) + other[...].astype(jnp.float32)
    )
    ffn_in = (rms_scale(hidden) * gain[...]).astype(jnp.bfloat16)
    first = place.core == 0
    kept[...] = jnp.where(first, hidden[:, :half], hidden[:, half:])
    every[0, me] = jnp.where(first, ffn_in[:, :half], ffn_in[:, half:])
    every[1, me] = jnp.where(first, ffn_in[:, half:], ffn_in[:, :half])

    def slot(db, da, dz):
        return ((db % side) * side + da % side) * line + dz % line

    used = [0]

    def pass_on(off, step):
        block = every.at[0, place.at(*off)]
        there = slot(*(o - s for o, s in zip(off, step)))
        send(block, block, link_send.at[used[0]], link_recv.at[there], place.near(*step))
        used[0] += 1

    def arrived(off):
        block = every.at[0, place.at(*off)]
        at = slot(*off)
        pltpu.make_async_copy(block, block, link_recv.at[at]).wait()
        send(block, every.at[1, place.at(*off)], core_send.at[at], core_recv.at[at], place.sibling())

    for dz in place.z_order():
        pass_on((0, 0, 0), (0, 0, dz))
    zs = [0] + place.z_order()
    for dz in zs:
        if dz:
            arrived((0, 0, dz))
        for d in range(1, side):
            pass_on((0, 0, dz), (0, d, 0))
        for d in range(1, side):
            pass_on((0, 0, dz), (d, 0, 0))
    for dz in zs:
        for da in range(1, side):
            arrived((0, da, dz))
            for d in range(1, side):
                pass_on((0, da, dz), (d, 0, 0))
    for dz in zs:
        for da in range(side):
            for db in range(1, side):
                arrived((db, da, dz))
    for d in range(1, ep_count):
        source = (me + ep_count - d) % ep_count
        pltpu.make_async_copy(notes.at[source], notes.at[source], note_recv.at[d - 1]).wait()
    for at in range(1, ep_count):
        dz, rest = at % line, at // line
        source = place.at(rest // side, rest % side, dz, 1 - place.core)
        block = every.at[1, source]
        pltpu.make_async_copy(block, block, core_recv.at[at]).wait()
    for copy in sends:
        copy.wait_send()


def spread(partial, stream, gain, meta):
    ep_count = lax.axis_size("ep")
    rows, width = stream.shape
    half = width // 2
    vmem = pl.BlockSpec(memory_space=pltpu.VMEM)
    dma = pltpu.SemaphoreType.DMA
    return pl.pallas_call(
        functools.partial(spread_kernel, ep_count),
        out_shape=(
            jax.ShapeDtypeStruct((2, ep_count, rows, half), jnp.bfloat16),
            jax.ShapeDtypeStruct((ep_count,) + meta.shape, jnp.float32),
            jax.ShapeDtypeStruct((rows, half), jnp.float32),
        ),
        in_specs=[vmem] * 4,
        out_specs=(vmem,) * 3,
        scratch_shapes=[
            pltpu.VMEM((rows, width), jnp.bfloat16),
            dma, dma,
            dma((ep_count,)), dma((ep_count,)),
            dma((ep_count,)), dma((ep_count,)),
            dma((ep_count,)), dma((ep_count,)),
        ],
        compiler_params=pltpu.CompilerParams(
            collective_id=1, has_side_effects=True, vmem_limit_bytes=grant(ep_count)
        ),
        name="spread",
    )(partial, stream, gain, meta)


def collect_kernel(ep_count, own, theirs, kept, out, held, total, from_b, from_a, from_z, *sems):
    core_send, core_recv, link_send, recv_b, recv_a, recv_z = sems
    place = Place(ep_count)
    side, line = place.side, place.line
    greet([place.sibling()] + place.partners())
    zs = place.z_order() + [0]
    spots = [(db, da, dz) for dz in zs for da in range(side) for db in range(1, side)]
    spots += [(0, da, dz) for dz in zs for da in range(1, side)]
    spots += [(0, 0, dz) for dz in zs]
    sends = []

    def send(src, dst, send_sem, recv_sem, target):
        copy = pltpu.make_async_remote_copy(
            src_ref=src, dst_ref=dst, send_sem=send_sem, recv_sem=recv_sem,
            device_id=target, device_id_type=MESH,
        )
        copy.start()
        sends.append(copy)

    for at, off in enumerate(spots):
        send(
            theirs.at[place.at(*off, 1 - place.core)], held.at[at],
            core_send.at[at], core_recv.at[at], place.sibling(),
        )

    def take(ref, sem):
        pltpu.make_async_copy(ref, ref, sem).wait()
        return ref[...].astype(jnp.float32)

    for at, (db, da, dz) in enumerate(spots):
        value = own[place.at(db, da, dz)].astype(jnp.float32)
        value = value + take(held.at[at], core_recv.at[at])
        if db:
            total[at] = value.astype(jnp.bfloat16)
            send(
                total.at[at], from_b.at[db - 1, da, dz],
                link_send.at[at], recv_b.at[db - 1, da, dz], place.near(db, 0, 0),
            )
            continue
        for d in range(1, side):
            value = value + take(from_b.at[d - 1, da, dz], recv_b.at[d - 1, da, dz])
        if da:
            total[at] = value.astype(jnp.bfloat16)
            send(
                total.at[at], from_a.at[da - 1, dz],
                link_send.at[at], recv_a.at[da - 1, dz], place.near(0, da, 0),
            )
            continue
        for d in range(1, side):
            value = value + take(from_a.at[d - 1, dz], recv_a.at[d - 1, dz])
        if dz:
            total[at] = value.astype(jnp.bfloat16)
            send(
                total.at[at], from_z.at[dz - 1],
                link_send.at[at], recv_z.at[dz - 1], place.near(0, 0, dz),
            )
            continue
        for d in range(1, line):
            value = value + take(from_z.at[d - 1], recv_z.at[d - 1])
        out[...] = (kept[...] + value).astype(out.dtype)
    for copy in sends:
        copy.wait_send()


def collect(own, theirs, kept):
    ep_count = lax.axis_size("ep")
    side, line = grid_of(ep_count)
    rows, half = kept.shape
    vmem = pl.BlockSpec(memory_space=pltpu.VMEM)
    dma = pltpu.SemaphoreType.DMA
    more = max(side - 1, 1)
    block = (rows, half)
    return pl.pallas_call(
        functools.partial(collect_kernel, ep_count),
        out_shape=jax.ShapeDtypeStruct((rows, half), jnp.bfloat16),
        in_specs=[vmem] * 3,
        out_specs=vmem,
        scratch_shapes=[
            pltpu.VMEM((ep_count,) + block, jnp.bfloat16),
            pltpu.VMEM((ep_count,) + block, jnp.bfloat16),
            pltpu.VMEM((more, side, line) + block, jnp.bfloat16),
            pltpu.VMEM((more, line) + block, jnp.bfloat16),
            pltpu.VMEM((max(line - 1, 1),) + block, jnp.bfloat16),
            dma((ep_count,)), dma((ep_count,)), dma((ep_count,)),
            dma((more, side, line)), dma((more, line)), dma((max(line - 1, 1),)),
        ],
        compiler_params=pltpu.CompilerParams(
            collective_id=2, has_side_effects=True, vmem_limit_bytes=grant(ep_count)
        ),
        name="collect",
    )(own.reshape((ep_count,) + block), theirs.reshape((ep_count,) + block), kept)


def grant(ep_count):
    return max(8, ep_count // 2) * 1024 * 1024


def local(
    stream,
    mixer_gain,
    gate_proj,
    input_proj,
    state_maps,
    step_proj,
    step_bias,
    decay_rate,
    input_taps,
    map_taps,
    input_past,
    map_past,
    head_state,
    skip_gain,
    inner_gain,
    mixer_out,
    channel_gain,
    expert_ids,
    expert_weight,
    expert_gate,
    expert_up,
    expert_down,
    dense_gate,
    dense_up,
    dense_down,
    dense_mix,
):
    core = lax.axis_index("tp")
    first = core == 0
    swap = [(0, 1), (1, 0)]
    units = dense_gate.shape[1] // 2

    def mine(left, right):
        return jnp.where(first, left, right)

    low = jnp.concatenate([dense_gate[:, :units], dense_up[:, :units]], axis=1)
    high = jnp.concatenate([dense_gate[:, units:], dense_up[:, units:]], axis=1)
    wide_own = mine(low, high)
    wide_other = lax.ppermute(mine(high, low), "tp", swap)
    down_own = mine(dense_down[:units], dense_down[units:])
    down_other = lax.ppermute(mine(dense_down[units:], dense_down[:units]), "tp", swap)
    mix_other = lax.ppermute(dense_mix, "tp", swap)

    inner_out, state_out = mix_heads(
        stream, mixer_gain, gate_proj, input_proj, state_maps, step_proj, step_bias, decay_rate,
        input_taps, map_taps, input_past, map_past, head_state, skip_gain, inner_gain,
    )
    partial_out = jnp.dot(inner_out, mixer_out, preferred_element_type=jnp.float32)

    row_count, width = stream.shape
    half = width // 2
    named = expert_ids[:, :, None] == jnp.arange(EXPERTS, dtype=jnp.int32)
    weight = jnp.sum(jnp.where(named, expert_weight[:, :, None], 0.0), axis=1)
    hits = jnp.any(named, axis=1)
    earlier = jnp.tril(jnp.ones((row_count, row_count), jnp.bfloat16), -1)
    rank = jnp.dot(earlier, hits.astype(jnp.bfloat16), preferred_element_type=jnp.float32)
    rank = jnp.where(hits, rank, -1.0)
    lanes = -(-2 * row_count // 128) * 128
    meta = jnp.concatenate([rank.T, weight.T], axis=1)
    meta = jnp.pad(meta, ((0, 0), (0, lanes - 2 * row_count)))

    every, notes, kept = spread(
        partial_out.astype(jnp.bfloat16), stream, channel_gain[None, :], meta
    )

    ep_count = lax.axis_size("ep")
    total_rows = ep_count * row_count
    slots = ep_count * CAP
    expert = lax.axis_index("ep") // (ep_count // EXPERTS)
    notes = lax.dynamic_index_in_dim(notes, expert, 1, keepdims=False)
    rank_all = notes[:, :row_count].reshape(1, total_rows)
    weight_all = notes[:, row_count : 2 * row_count].reshape(1, total_rows)
    slot_ids = jnp.arange(slots, dtype=jnp.int32)[:, None]
    row_ids = jnp.arange(total_rows, dtype=jnp.int32)[None, :]
    match = (slot_ids // CAP == row_ids // row_count) & (
        (slot_ids % CAP).astype(jnp.float32) == rank_all
    )
    slot_weight = jnp.sum(jnp.where(match, weight_all, 0.0), axis=1, keepdims=True)
    pick = match.astype(jnp.bfloat16)
    all_own = every[0].reshape(total_rows, half)
    all_other = every[1].reshape(total_rows, half)

    def f32_dot(left, right):
        return jnp.dot(left, right, preferred_element_type=jnp.float32)

    rows_own = f32_dot(pick, all_own).astype(jnp.bfloat16)
    rows_other = f32_dot(pick, all_other).astype(jnp.bfloat16)
    rows = jnp.concatenate([mine(rows_own, rows_other), mine(rows_other, rows_own)], axis=1)
    act = (jax.nn.silu(f32_dot(rows, expert_gate)) * f32_dot(rows, expert_up)).astype(jnp.bfloat16)
    share = (f32_dot(act, expert_down) * slot_weight).astype(jnp.bfloat16)
    share_own = mine(share[:, :half], share[:, half:])
    share_other = mine(share[:, half:], share[:, :half])

    wide = f32_dot(all_own, wide_own) + f32_dot(all_other, wide_other)
    dense_act = (jax.nn.silu(wide[:, :units]) * wide[:, units:]).astype(jnp.bfloat16)

    def result(share_half, down_half, mix_half):
        spread_back = lax.dot_general(
            pick, share_half, (((0,), (0,)), ((), ())), preferred_element_type=jnp.float32
        )
        dense = f32_dot(dense_act, down_half) * jax.nn.sigmoid(mix_half)
        return (spread_back + dense).astype(jnp.bfloat16)

    updated = collect(
        result(share_own, down_own, dense_mix),
        result(share_other, down_other, mix_other),
        kept,
    )
    return (updated, state_out)


def solution(mesh):
    placed = (
        P("ep", None),
        P(),
        P(None, "tp"),
        P(None, "tp"),
        P(None, None, "tp"),
        P(None, "tp"),
        P("tp"),
        P("tp"),
        P(None, "tp"),
        P(None, None, "tp"),
        P("ep", None, "tp"),
        P("ep", None, None, "tp"),
        P("ep", "tp", None),
        P("tp"),
        P("tp"),
        P("tp", None),
        P(),
        P("ep", None),
        P("ep", None),
        P(None, ("ep", "tp")),
        P(None, ("ep", "tp")),
        P(("ep", "tp"), None),
        P("tp", "ep"),
        P("tp", "ep"),
        P("ep", "tp"),
        P("tp"),
    )
    return jax.shard_map(
        local,
        mesh=mesh,
        in_specs=placed,
        out_specs=(P("ep", "tp"), P("ep", "tp", None)),
        check_vma=False,
    )
```
